512 devices in a mesh: sp: 64 (over z, y), tp: 8 (over x, core).
Axes of the slice: x: 4, y: 4, z: 16, core: 2. Of those that a mesh axis runs over, the one named last changes fastest.
Arguments:
- prompt: bfloat16 [64, 1024, 2048], P('sp', None, 'tp'), may hold values from -6 to 6
- new_input: bfloat16 [64, 2048], P('sp', 'tp'), may hold values from -140 to 140
- w_query: bfloat16 [2048, 2048], P('sp', 'tp'), may hold values from -0.21875 to 0.21875
- w_key: bfloat16 [2048, 2048], P('sp', 'tp'), may hold values from -0.125 to 0.125
- w_value: bfloat16 [2048, 2048], P('sp', 'tp'), may hold values from -0.125 to 0.125
- lam: float32 [16], P('tp'), may hold values from 0.3 to 0.8
- out_gain: float32 [128], replicated, may hold values from 0.1 to 1.9
Outputs:
- key_cache: bfloat16 [64, 1024, 2048], P('sp', None, 'tp')
- value_cache: bfloat16 [64, 1024, 2048], P('sp', None, 'tp')
- first_read: bfloat16 [64, 16, 128], P('sp', 'tp')
The draws below stay inside these ranges and needn't reach their ends.
All inputs are finite; a program needn't handle non-finite values.
Results may differ from the reference program's by a relative error of at most 0.02.
The reference program's roundings to bfloat16 on the way (of `query`) count: a program that leaves them out, or rounds other values in their place, can miss the bound.
Values may be sent and summed in bfloat16 or wider, within the bound.
No kernel may reach another device: no remote copies, remote signals or barrier semaphores. Data moves between devices by JAX's collectives and lax.ppermute only.
A program may use at most 64 MiB of HBM per device.

```python
import jax
import jax.numpy as jnp
from jax import lax

WIDTH = 2048
HEADS = 16
MAP_DIM = 64
VAL_DIM = 128
LEN = 1024
SEQS = 64


def draw_new_input(key, part):
    values = jax.random.normal(key, (SEQS, WIDTH), jnp.float32)
    values = jnp.clip(values, -6.0, 6.0)
    return values.astype(jnp.bfloat16)


def levels(own_key, dims, shards, low, largest):
    gain = 1.0
    for dim, blocks in shards:
        draws = jax.random.uniform(jax.random.fold_in(jax.random.fold_in(own_key, 6), dim), (blocks,), jnp.float32, low / len(shards), largest / len(shards))
        gain = gain * jnp.repeat(jnp.exp(draws), dims[dim] // blocks).reshape((-1,) + (1,) * (len(dims) - 1 - dim))
    return gain


def gaussian(own_key, shape, width, reach, split=(), kind=jnp.bfloat16):
    level = levels(own_key, shape, split, -0.22, 0.18) if split else 1.0
    drawn = jax.random.normal(own_key, shape, jnp.float32) * width * level
    return jnp.minimum(jnp.maximum(drawn, -reach), reach).astype(kind)


def setup_inputs(seed: int = 0) -> dict:
    streams_of = jax.random.split(jax.random.key(seed), 8)
    prompt = gaussian(streams_of[0], (SEQS, LEN, WIDTH), 1.0, 6.0, ((0, 64), (2, 8)))
    new_input = draw_new_input(jax.random.fold_in(streams_of[7], 71), 0)
    w_query = gaussian(streams_of[2], (WIDTH, HEADS * 2 * MAP_DIM), (WIDTH // 3) ** -0.5, 0.21875, ((0, 64), (1, 8)))
    w_key = gaussian(streams_of[3], (WIDTH, HEADS * 2 * MAP_DIM), WIDTH ** -0.5, 0.125, ((0, 64), (1, 8)))
    w_value = gaussian(streams_of[4], (WIDTH, HEADS * VAL_DIM), WIDTH ** -0.5, 0.125, ((0, 64), (1, 8)))
    lam = jnp.clip(0.3 + 0.5 * jax.random.uniform(streams_of[5], (HEADS,), jnp.float32) ** levels(streams_of[5], (HEADS,), ((0, 8),), -0.2, 0.2), 0.3, 0.8)
    out_gain = jnp.clip(1.0 + 0.18 * jax.random.normal(streams_of[6], (VAL_DIM,), jnp.float32), 0.1, 1.9)
    return {"prompt": prompt, "new_input": new_input, "w_query": w_query, "w_key": w_key, "w_value": w_value, "lam": lam, "out_gain": out_gain}


rope_base = 500000.0
norm_eps = 1e-05

def rotate(vectors, angle):
    half = vectors.shape[-1] // 2
    cosine_table = jnp.cos(angle)
    sine = jnp.sin(angle)
    first = vectors[..., :half]
    second = vectors[..., half:]
    return jnp.concatenate([first * cosine_table - second * sine, second * cosine_table + first * sine], axis=-1)

def inverse_freq():
    return rope_base ** (-(jnp.arange(MAP_DIM // 2, dtype=jnp.float32) * 2.0 / MAP_DIM))

def reference(prompt, new_input, w_query, w_key, w_value, lam, out_gain):
    rows = prompt.reshape(SEQS * LEN, WIDTH)
    inverse = inverse_freq()
    positions = jnp.arange(LEN, dtype=jnp.float32)
    keys = jnp.dot(rows, w_key, preferred_element_type=jnp.float32).reshape(SEQS, LEN, HEADS, 2, MAP_DIM)
    keys = rotate(keys, positions[:, None, None, None] * inverse).astype(jnp.bfloat16)
    values = jnp.dot(rows, w_value, preferred_element_type=jnp.float32).astype(jnp.bfloat16)
    values = values.reshape(SEQS, LEN, HEADS, VAL_DIM)
    query = jnp.dot(new_input, w_query, preferred_element_type=jnp.float32).reshape(SEQS, HEADS, 2, MAP_DIM)
    query = rotate(query, jnp.float32(LEN) * inverse).astype(jnp.bfloat16)

    def single_sequence(args):
        single_head_query, single_head_keys, single_head_values = args
        attention_scores = jnp.einsum('fke,afke->fka', single_head_query.astype(jnp.float32), single_head_keys.astype(jnp.float32))
        weights = jax.nn.softmax(attention_scores * MAP_DIM ** (-0.5), axis=-1)
        mixed = jnp.einsum('hml,lhe->hme', weights, single_head_values.astype(jnp.float32), precision=lax.Precision.HIGHEST)
        diff = mixed[:, 0] - lam[:, None] * mixed[:, 1]
        normed = diff * lax.rsqrt(lax.optimization_barrier(jnp.mean(diff * diff, axis=-1, keepdims=True)) + norm_eps)
        return (normed * out_gain).astype(jnp.bfloat16)
    first_read = lax.map(single_sequence, (query, keys, values))
    return (keys.reshape(SEQS, LEN, HEADS * 2 * MAP_DIM), values.reshape(SEQS, LEN, HEADS * VAL_DIM), first_read)
```

```python
import functools

import jax
import jax.numpy as jnp
from jax import lax
from jax.experimental import pallas as pl
from jax.experimental.pallas import tpu as pltpu
from jax.sharding import Mesh
from jax.sharding import PartitionSpec as P

MAP_DIM = 64
VAL_DIM = 128
LEN = 1024
HALF = LEN // 2
PAD = 8
ROWS = 256
rope_base = 500000.0
norm_eps = 1e-05


def inverse_freq():
    return rope_base ** (-(jnp.arange(MAP_DIM // 2, dtype=jnp.float32) * 2.0 / MAP_DIM))


def tables(positions):
    angle = positions[:, None] * inverse_freq()
    cosine, sine = jnp.cos(angle), jnp.sin(angle)
    return jnp.tile(cosine, (1, 4)), jnp.tile(jnp.concatenate([-sine, sine], axis=1), (1, 2))


def shift(value, axis, by):
    n = lax.axis_size(axis)
    return lax.ppermute(value, axis, [(i, (i + by) % n) for i in range(n)])


def rotated(t, cosine, sine):
    lane = lax.broadcasted_iota(jnp.int32, t.shape, 1)
    partner = jnp.where(lane % MAP_DIM < MAP_DIM // 2, pltpu.roll(t, 128 - 32, 1), pltpu.roll(t, 32, 1))
    return t * cosine + partner * sine


def kernel(order, lam, own_p, far_p, own_c, far_c, weights, cos_t, sin_t, cos_q, sin_q, gain, keys, values, read, w):
    width = weights.shape[2]
    for j in range(8):
        t = order[j]
        for z in range(2):
            for y in range(4):
                row = pl.multiple_of((2 * t + z) * 32, 32)
                w[256 * j + 32 * (4 * z + y) : 256 * j + 32 * (4 * z + y) + 32, :] = weights[y, pl.ds(row, 32), :]

    def rows_of(lo, n):
        parts = [own_p[lo : lo + n, :]] + [far_p[k, lo : lo + n, :] for k in range(3)]
        parts += [own_c[lo : lo + n, :]] + [far_c[k, lo : lo + n, :] for k in range(3)]
        return jnp.concatenate(parts, axis=1)

    for m in range(LEN // ROWS):
        lo = m * ROWS
        both = jnp.dot(rows_of(lo, ROWS), w[:, 256:width], preferred_element_type=jnp.float32)
        cosine, sine = cos_t[lo : lo + ROWS, :], sin_t[lo : lo + ROWS, :]
        for h in range(2):
            part = both[:, 128 * h : 128 * h + 128]
            keys[lo : lo + ROWS, 128 * h : 128 * h + 128] = rotated(part, cosine, sine).astype(jnp.bfloat16)
        values[lo : lo + ROWS, :] = both[:, 256:512].astype(jnp.bfloat16)

    q = jnp.dot(rows_of(LEN, PAD), w[:, 0:256], preferred_element_type=jnp.float32)
    q = jnp.concatenate([rotated(q[:, 128 * h : 128 * h + 128], cos_q[...], sin_q[...]) for h in range(2)], axis=1)
    q = jnp.broadcast_to(q[0:1, :], (8, 256))
    row = lax.broadcasted_iota(jnp.int32, (8, 256), 0)
    lane = lax.broadcasted_iota(jnp.int32, (8, 256), 1)
    q = jnp.where(lane // MAP_DIM == row, q, 0.0).astype(jnp.bfloat16)
    scores = lax.dot_general(q, keys[...], (((1,), (1,)), ((), ())), preferred_element_type=jnp.float32)
    scores = scores * MAP_DIM ** (-0.5)
    e = jnp.exp(scores - jnp.max(scores, axis=1, keepdims=True))
    total = jnp.sum(e, axis=1, keepdims=True)
    high = e.astype(jnp.bfloat16)
    low = (e - high.astype(jnp.float32)).astype(jnp.bfloat16)
    v = values[...]
    mixed = jnp.dot(high, v, preferred_element_type=jnp.float32) + jnp.dot(low, v, preferred_element_type=jnp.float32)
    mixed = mixed / total
    for h in range(2):
        cols = mixed[:, VAL_DIM * h : VAL_DIM * h + VAL_DIM]
        diff = cols[2 * h : 2 * h + 1, :] - lam[h] * cols[2 * h + 1 : 2 * h + 2, :]
        normed = diff * lax.rsqrt(jnp.mean(diff * diff, axis=1, keepdims=True) + norm_eps)
        read[h : h + 1, :] = (normed * gain[...]).astype(jnp.bfloat16)


def compute(order, lam, arrays):
    vmem = pl.BlockSpec(memory_space=pltpu.VMEM)
    smem = pl.BlockSpec(memory_space=pltpu.SMEM)
    return pl.pallas_call(
        kernel,
        in_specs=[smem, smem] + [vmem] * len(arrays),
        out_specs=[vmem] * 3,
        out_shape=[
            jax.ShapeDtypeStruct((LEN, 256), jnp.bfloat16),
            jax.ShapeDtypeStruct((LEN, 256), jnp.bfloat16),
            jax.ShapeDtypeStruct((2, VAL_DIM), jnp.bfloat16),
        ],
        scratch_shapes=[pltpu.VMEM((2048, 768), jnp.bfloat16)],
        compiler_params=pltpu.CompilerParams(vmem_limit_bytes=40 * 1024 * 1024),
        name="project_and_read",
    )(order, lam, *arrays)


def body(prompt, new_input, w_query, w_key, w_value, lam, out_gain):
    own = jnp.concatenate([prompt[0], jnp.pad(new_input, ((0, PAD - 1), (0, 0)))], axis=0)
    one = shift(own, "x", 1)
    three = shift(own, "x", -1)
    two = jnp.concatenate([shift(own[:HALF], "x", 2), shift(own[HALF:], "x", -2)], axis=0)
    far = jnp.stack([one, two, three])
    own_c = shift(own, "c", 1)
    far_c = shift(far, "c", 1)

    mine = jnp.concatenate([w_query, w_key, w_value], axis=1)
    column = lax.all_gather(mine, "z", axis=0, tiled=True)
    weights = lax.all_to_all(jnp.broadcast_to(column, (4, *column.shape)), "y", 0, 0, tiled=True)

    ix, ic = lax.axis_index("x"), lax.axis_index("c")
    order = jnp.stack([2 * ((ix - d) % 4) + c for c in (ic, 1 - ic) for d in range(4)]).astype(jnp.int32)
    cos_t, sin_t = tables(jnp.arange(LEN, dtype=jnp.float32))
    cos_q, sin_q = tables(jnp.full((1,), LEN, jnp.float32))
    keys, values, read = compute(
        order, lam, (own, far, own_c, far_c, weights, cos_t, sin_t, cos_q, sin_q, out_gain[None])
    )
    return keys[None], values[None], read[None]


def solution(mesh):
    split = Mesh(mesh.devices.reshape(16, 4, 4, 2), ("z", "y", "x", "c"))
    sp, tp = ("z", "y"), ("x", "c")
    in_specs = (P(sp, None, tp), P(sp, tp), P(sp, tp), P(sp, tp), P(sp, tp), P(tp), P())
    out_specs = (P(sp, None, tp), P(sp, None, tp), P(sp, tp, None))
    return jax.shard_map(body, mesh=split, in_specs=in_specs, out_specs=out_specs, check_vma=False)
```

```python
import jax
import jax.numpy as jnp
from jax import lax
from jax.experimental import pallas as pl
from jax.experimental.pallas import tpu as pltpu
from jax.sharding import Mesh
from jax.sharding import PartitionSpec as P


MAP_DIM = 64
VAL_DIM = 128
LEN = 1024
PAD = 8
ROWS = 256
rope_base = 500000.0
norm_eps = 1e-05


def inverse_freq():
    return rope_base ** (-(jnp.arange(MAP_DIM // 2, dtype=jnp.float32) * 2.0 / MAP_DIM))


def tables(positions):
    inverse = inverse_freq()
    angle = positions[:, None] * jnp.tile(inverse, 4)[None, :]
    sign = jnp.where(jnp.arange(128) % MAP_DIM < MAP_DIM // 2, -1.0, 1.0)
    return jnp.cos(angle), jnp.sin(angle) * sign[None, :]


def shift(value, axis, by):
    n = lax.axis_size(axis)
    return lax.ppermute(value, axis, [(i, (i + by) % n) for i in range(n)])


def rotated(t, cosine, sine):
    lane = lax.broadcasted_iota(jnp.int32, t.shape, 1)
    partner = jnp.where(lane % MAP_DIM < MAP_DIM // 2, pltpu.roll(t, 128 - 32, 1), pltpu.roll(t, 32, 1))
    return t * cosine + partner * sine


def kernel(order, lam, a0, a1, a2, a3, b0, b1, b2, b3, weights, cos_t, sin_t, cos_q, sin_q, gain, keys, values, read, w):
    width = weights.shape[2]
    for j in range(8):
        t = order[j]
        for z in range(2):
            for y in range(4):
                row = pl.multiple_of((2 * t + z) * 32, 32)
                w[256 * j + 32 * (4 * z + y) : 256 * j + 32 * (4 * z + y) + 32, :] = weights[y, pl.ds(row, 32), :]

    def rows_of(lo, n):
        return jnp.concatenate([p[lo : lo + n, :] for p in (a0, a1, a2, a3, b0, b1, b2, b3)], axis=1)

    for m in range(LEN // ROWS):
        lo = m * ROWS
        both = jnp.dot(rows_of(lo, ROWS), w[:, 256:width], preferred_element_type=jnp.float32)
        cosine, sine = cos_t[lo : lo + ROWS, :], sin_t[lo : lo + ROWS, :]
        for h in range(2):
            part = both[:, 128 * h : 128 * h + 128]
            keys[lo : lo + ROWS, 128 * h : 128 * h + 128] = rotated(part, cosine, sine).astype(jnp.bfloat16)
        values[lo : lo + ROWS, :] = both[:, 256:512].astype(jnp.bfloat16)

    q = jnp.dot(rows_of(LEN, PAD), w[:, 0:256], preferred_element_type=jnp.float32)
    q = jnp.concatenate([rotated(q[:, 128 * h : 128 * h + 128], cos_q[...], sin_q[...]) for h in range(2)], axis=1)
    q = jnp.broadcast_to(q[0:1, :], (8, 256))
    row = lax.broadcasted_iota(jnp.int32, (8, 256), 0)
    lane = lax.broadcasted_iota(jnp.int32, (8, 256), 1)
    q = jnp.where(lane // MAP_DIM == row, q, 0.0).astype(jnp.bfloat16)
    scores = lax.dot_general(q, keys[...], (((1,), (1,)), ((), ())), preferred_element_type=jnp.float32)
    scores = scores * MAP_DIM ** (-0.5)
    e = jnp.exp(scores - jnp.max(scores, axis=1, keepdims=True))
    total = jnp.sum(e, axis=1, keepdims=True)
    high = e.astype(jnp.bfloat16)
    low = (e - high.astype(jnp.float32)).astype(jnp.bfloat16)
    v = values[...]
    mixed = jnp.dot(high, v, preferred_element_type=jnp.float32) + jnp.dot(low, v, preferred_element_type=jnp.float32)
    mixed = mixed / total
    for h in range(2):
        cols = mixed[:, VAL_DIM * h : VAL_DIM * h + VAL_DIM]
        diff = cols[2 * h : 2 * h + 1, :] - lam[h] * cols[2 * h + 1 : 2 * h + 2, :]
        normed = diff * lax.rsqrt(jnp.mean(diff * diff, axis=1, keepdims=True) + norm_eps)
        read[h : h + 1, :] = (normed * gain[...]).astype(jnp.bfloat16)


def compute(order, lam, arrays):
    vmem = pl.BlockSpec(memory_space=pltpu.VMEM)
    smem = pl.BlockSpec(memory_space=pltpu.SMEM)
    return pl.pallas_call(
        kernel,
        in_specs=[smem, smem] + [vmem] * len(arrays),
        out_specs=[vmem] * 3,
        out_shape=[
            jax.ShapeDtypeStruct((LEN, 256), jnp.bfloat16),
            jax.ShapeDtypeStruct((LEN, 256), jnp.bfloat16),
            jax.ShapeDtypeStruct((2, VAL_DIM), jnp.bfloat16),
        ],
        scratch_shapes=[pltpu.VMEM((2048, 768), jnp.bfloat16)],
        compiler_params=pltpu.CompilerParams(vmem_limit_bytes=40 * 1024 * 1024),
        name="project_and_read",
    )(order, lam, *arrays)


def body(prompt, new_input, w_query, w_key, w_value, lam, out_gain):
    mine = jnp.concatenate([w_query, w_key, w_value], axis=1)
    column = lax.all_gather(mine, "z", axis=0, tiled=True)
    weights = lax.all_to_all(jnp.broadcast_to(column, (4, *column.shape)), "y", 0, 0, tiled=True)

    own = jnp.concatenate([prompt[0], jnp.pad(new_input, ((0, PAD - 1), (0, 0)))], axis=0)
    near = [own]
    for d in range(1, 4):
        near.append(shift(own, "x", d))
    partner = [shift(p, "c", 1) for p in near]

    ix, ic = lax.axis_index("x"), lax.axis_index("c")
    order = jnp.stack([2 * ((ix - d) % 4) + c for c in (ic, 1 - ic) for d in range(4)]).astype(jnp.int32)
    cos_t, sin_t = tables(jnp.arange(LEN, dtype=jnp.float32))
    cos_q, sin_q = tables(jnp.full((1,), LEN, jnp.float32))
    keys, values, read = compute(
        order, lam, (*near, *partner, weights, cos_t, sin_t, cos_q, sin_q, out_gain[None])
    )
    return keys[None], values[None], read[None]


def solution(mesh):
    split = Mesh(mesh.devices.reshape(16, 4, 4, 2), ("z", "y", "x", "c"))
    sp, tp = ("z", "y"), ("x", "c")
    in_specs = (P(sp, None, tp), P(sp, tp), P(sp, tp), P(sp, tp), P(sp, tp), P(tp), P())
    out_specs = (P(sp, None, tp), P(sp, None, tp), P(sp, tp, None))
    return jax.shard_map(body, mesh=split, in_specs=in_specs, out_specs=out_specs, check_vma=False)
```
